32 devices in a mesh: fs: 8 (over z, core), tp: 4 (over y, x).
Axes of the slice: x: 2, y: 2, z: 4, core: 2. Of those that a mesh axis runs over, the one named last changes fastest.
Arguments:
- tokens: bfloat16 [4096, 2048], P('fs'), may hold values from -6 to 6
- cotangent: bfloat16 [4096, 2048], P('fs'), may hold values from -6 to 6
- gate_weight: bfloat16 [2048, 2816], P('fs', 'tp'), may hold values from -0.125 to 0.125
- up_weight: bfloat16 [2048, 2816], P('fs', 'tp'), may hold values from -0.125 to 0.125
- down_weight: bfloat16 [2048, 2816], P('fs', 'tp'), may hold values from -0.109375 to 0.109375
Outputs:
- input_grad: bfloat16 [4096, 2048], P('fs', 'tp')
- gate_grad: float32 [2048, 2816], P('fs', 'tp')
- up_grad: float32 [2048, 2816], P('fs', 'tp')
- down_grad: float32 [2048, 2816], P('fs', 'tp')
The draws below stay inside these ranges and needn't reach their ends.
All inputs are finite; a program needn't handle non-finite values.
Results may differ from the reference program's by a relative error of at most 0.014.
Values may be sent and summed in bfloat16 or wider, within the bound.
A program may use at most 64 MiB of HBM per device.

```python
import jax
import jax.numpy as jnp
from jax import lax

D = 2048
FF = 2816
TOKENS = 4096
N_TP = 4


def with_spikes(array, own_key, source, target, shards_of, factor):
    owner, partner = [(jnp.arange(array.shape[position]) // (array.shape[position] // shards_of)).reshape([-1 if axis == position else 1 for axis in range(array.ndim)]) for position in (source, target)]
    chosen = jax.random.permutation(own_key, shards_of)[partner]
    strong = (owner == chosen) | (owner == (partner + shards_of // 2) % shards_of)
    return jnp.where(strong, factor * array, array)


def block_levels(stream_key, dims, split, smallest, high):
    def one(position, shards_of):
        draws = jax.random.uniform(jax.random.fold_in(jax.random.fold_in(stream_key, 6), position), (shards_of,), jnp.float32, smallest / len(split), high / len(split))
        return jnp.repeat(jnp.exp(draws), dims[position] // shards_of).reshape((-1,) + (1,) * (len(dims) - position - 1))

    gain = one(*split[0])
    for cut in split[1:]:
        gain = gain * one(*cut)
    return gain


def centred(stream_key, extent, scale, limit, pieces=(), kind=jnp.bfloat16):
    values = jax.random.normal(stream_key, extent, jnp.float32) * scale
    if len(pieces) > 0:
        values = block_levels(stream_key, extent, pieces, -0.22, 0.18) * values
    return jnp.clip(values, min=-limit, max=limit).astype(kind)


def heavy_noise(stream_key, dims, scale, most, pieces, heavy, kind=jnp.bfloat16):
    drawn = scale * jax.random.normal(stream_key, dims, jnp.float32)
    if pieces:
        drawn = drawn * block_levels(stream_key, dims, pieces, -0.22, 0.18)
    return jnp.clip(with_spikes(drawn, jax.random.fold_in(stream_key, 3), *heavy), -most, most).astype(kind)


def setup_inputs(seed: int = 0) -> dict:
    streams_of = jax.random.split(jax.random.key(seed), 6)
    tokens = centred(streams_of[0], (TOKENS, D), 1.0, 6.0, ((0, 8),))
    cotangent = heavy_noise(streams_of[1], (TOKENS, D), 1.0, 6.0, ((0, 8),), (0, 1, 8, 2.0))
    gate_weight = centred(streams_of[2], (D, FF), D ** -0.5, 0.125, ((0, 8), (1, 4)))
    up_weight = centred(streams_of[3], (D, FF), D ** -0.5, 0.125, ((0, 8), (1, 4)))
    down_weight = centred(streams_of[4], (D, FF), FF ** -0.5, 0.109375, ((0, 8), (1, 4)))
    return dict(tokens=tokens, cotangent=cotangent, gate_weight=gate_weight, up_weight=up_weight, down_weight=down_weight)


def reference(tokens, cotangent, gate_weight, up_weight, down_weight):
    gate = jnp.dot(tokens, gate_weight, preferred_element_type=jnp.float32)
    up = jnp.dot(tokens, up_weight, preferred_element_type=jnp.float32)
    sig = jax.nn.sigmoid(gate)
    act = gate * sig
    hidden = (act * up).astype(jnp.bfloat16)
    hidden_grad = lax.dot_general(cotangent, down_weight, (((1,), (0,)), ((), ())), preferred_element_type=jnp.float32)
    gate_cot = (hidden_grad * up * sig * (1.0 + gate * (1.0 - sig))).astype(jnp.bfloat16)
    up_cot = (hidden_grad * act).astype(jnp.bfloat16)
    width = FF // N_TP

    def add_block(total, index):
        start = (index * width).astype(jnp.int32)
        gate_part = lax.dynamic_slice_in_dim(gate_cot, start, width, 1)
        up_part = lax.dynamic_slice_in_dim(up_cot, start, width, 1)
        gate_rows = lax.dynamic_slice_in_dim(gate_weight, start, width, 1)
        up_rows = lax.dynamic_slice_in_dim(up_weight, start, width, 1)
        partial_value = lax.dot_general(gate_part, gate_rows, (((1,), (1,)), ((), ())), preferred_element_type=jnp.float32)
        partial_value = partial_value + lax.dot_general(up_part, up_rows, (((1,), (1,)), ((), ())), preferred_element_type=jnp.float32)
        rounded = lax.optimization_barrier(partial_value.astype(jnp.bfloat16))
        return total + rounded.astype(jnp.float32), None

    start_total = jnp.zeros((tokens.shape[0], tokens.shape[1]), jnp.float32)
    total, unused = lax.scan(add_block, start_total, jnp.arange(N_TP, dtype=jnp.int32))
    input_grad = total.astype(jnp.bfloat16)
    contract = (((0,), (0,)), ((), ()))
    gate_grad = lax.dot_general(tokens, gate_cot, contract, preferred_element_type=jnp.float32)
    up_grad = lax.dot_general(tokens, up_cot, contract, preferred_element_type=jnp.float32)
    down_grad = lax.dot_general(cotangent, hidden, contract, preferred_element_type=jnp.float32)
    return (input_grad, gate_grad, up_grad, down_grad)
```

```python
import functools

import jax
import jax.numpy as jnp
from jax import lax
from jax.experimental import pallas as pl
from jax.experimental.pallas import tpu as pltpu
from jax.sharding import PartitionSpec as P


def row_product(left, right):
    return lax.dot_general(
        left, right, (((1,), (1,)), ((), ())), preferred_element_type=jnp.float32
    )


def token_product(left, right):
    return lax.dot_general(
        left, right, (((0,), (0,)), ((), ())), preferred_element_type=jnp.float32
    )


def owner_sum(received, groups):
    return received.reshape(groups, received.shape[0] // groups, received.shape[1]).sum(axis=0)


def plain_shards(tokens, cotangent, gate_weight, up_weight, down_weight):
    groups = lax.axis_size("fs")
    whole_gate, whole_up, whole_down = (
        lax.all_gather(gate_weight, "fs", axis=0, tiled=True),
        lax.all_gather(up_weight, "fs", axis=0, tiled=True),
        lax.all_gather(down_weight, "fs", axis=0, tiled=True),
    )
    gate = jnp.dot(tokens, whole_gate, preferred_element_type=jnp.float32)
    up = jnp.dot(tokens, whole_up, preferred_element_type=jnp.float32)
    hidden_grad = jnp.dot(cotangent, whole_down, preferred_element_type=jnp.float32)
    sig = jax.nn.sigmoid(gate)
    act = gate * sig
    hidden = (act * up).astype(jnp.bfloat16)
    gate_cot = (hidden_grad * up * sig * (1.0 + gate * (1.0 - sig))).astype(jnp.bfloat16)
    up_cot = (hidden_grad * act).astype(jnp.bfloat16)
    partial_value = row_product(gate_cot, whole_gate) + row_product(up_cot, whole_up)
    input_grad = lax.psum_scatter(
        partial_value.astype(jnp.bfloat16), "tp", scatter_dimension=1, tiled=True
    )
    gate_term = token_product(tokens, gate_cot)
    gate_grad = owner_sum(
        lax.all_to_all(
            gate_term.astype(jnp.bfloat16), "fs", split_axis=0, concat_axis=0, tiled=True
        ).astype(gate_term.dtype),
        groups,
    )
    up_term = token_product(tokens, up_cot)
    up_grad = owner_sum(
        lax.all_to_all(
            up_term.astype(jnp.bfloat16), "fs", split_axis=0, concat_axis=0, tiled=True
        ).astype(up_term.dtype),
        groups,
    )
    down_term = token_product(cotangent, hidden)
    down_grad = owner_sum(
        lax.all_to_all(
            down_term.astype(jnp.bfloat16), "fs", split_axis=0, concat_axis=0, tiled=True
        ).astype(down_term.dtype),
        groups,
    )
    return (input_grad, gate_grad, up_grad, down_grad)


MESH = pl.DeviceIdType.MESH
GATE, UP, DOWN = 0, 1, 2
RIGHT, LEFT, SIBLING = 0, 1, 2


def kernel(
    n, n_tp, tok, cot, gw, uw, dw, ig_out, out,
    x, w_all, acc, cots, sib_out, sib_in, line_out, line_in, total, ig_part, ig_in,
    local_sem, ag_send, ag_recv, sib_send, sib_recv, line_send, line_recv, ig_send, ig_recv,
):
    me, tp = lax.axis_index("fs"), lax.axis_index("tp")
    z, c = me // 2, me % 2
    nz = n // 2
    other = 2 * z + 1 - c
    rows = gw.shape[0]
    own_columns = ig_out.shape[1]
    pieces = own_columns // rows
    has_left, has_right = z > 0, z < nz - 1
    is_end = jnp.logical_or(z == 0, z == nz - 1)

    loads = [
        pltpu.make_async_copy(gw, w_all.at[GATE, me], local_sem.at[0]),
        pltpu.make_async_copy(uw, w_all.at[UP, me], local_sem.at[1]),
        pltpu.make_async_copy(dw, w_all.at[DOWN, me], local_sem.at[2]),
        pltpu.make_async_copy(tok, x.at[0], local_sem.at[3]),
        pltpu.make_async_copy(cot, x.at[1], local_sem.at[4]),
    ]
    for load in loads:
        load.start()

    barrier = pltpu.get_barrier_semaphore()
    pl.semaphore_signal(barrier, inc=1, device_id={"fs": other}, device_id_type=MESH)
    for step in range(1, n_tp):
        pl.semaphore_signal(
            barrier, inc=1, device_id={"tp": lax.rem(tp + step, n_tp)}, device_id_type=MESH
        )

    @pl.when(has_right)
    def _():
        pl.semaphore_signal(barrier, inc=1, device_id={"fs": me + 2}, device_id_type=MESH)

    @pl.when(has_left)
    def _():
        pl.semaphore_signal(barrier, inc=1, device_id={"fs": me - 2}, device_id_type=MESH)

    pl.semaphore_wait(barrier, n_tp + has_left.astype(jnp.int32) + has_right.astype(jnp.int32))

    def gather_copy(w, chip, way):
        slot = 2 * chip + c
        device = (me + 2, me - 2, other)[way]
        return pltpu.make_async_remote_copy(
            src_ref=w_all.at[w, slot], dst_ref=w_all.at[w, slot],
            send_sem=ag_send.at[w, way, chip], recv_sem=ag_recv.at[w, slot],
            device_id={"fs": device}, device_id_type=MESH,
        )

    def gather_wait(w, slot):
        pltpu.make_async_remote_copy(
            src_ref=w_all.at[w, slot], dst_ref=w_all.at[w, slot],
            send_sem=ag_send.at[w, SIBLING, 0], recv_sem=ag_recv.at[w, slot],
            device_id={"fs": other}, device_id_type=MESH,
        ).wait_recv()

    for w in range(3):
        loads[w].wait()
        if w == 0:

            @pl.when(has_right)
            def _():
                gather_copy(GATE, z, RIGHT).start()

            @pl.when(has_left)
            def _():
                gather_copy(GATE, z, LEFT).start()

        gather_copy(w, z, SIBLING).start()
    acc[...] = jnp.zeros_like(acc)
    loads[3].wait()
    loads[4].wait()

    def gather_step(w, s):
        @pl.when(jnp.logical_and(s > 0, z - s >= 0))
        def _():
            gather_wait(w, me - 2 * s)

            @pl.when(has_right)
            def _():
                gather_copy(w, z - s, RIGHT).start()

            gather_copy(w, z - s, SIBLING).start()

        @pl.when(jnp.logical_and(s > 0, z + s < nz))
        def _():
            gather_wait(w, me + 2 * s)

            @pl.when(has_left)
            def _():
                gather_copy(w, z + s, LEFT).start()

            gather_copy(w, z + s, SIBLING).start()

        @pl.when(jnp.logical_and(w < DOWN, jnp.logical_and(has_right, s == z)))
        def _():
            gather_copy(w + 1, z, RIGHT).start()

        @pl.when(jnp.logical_and(w < DOWN, jnp.logical_and(has_left, s == nz - 1 - z)))
        def _():
            gather_copy(w + 1, z, LEFT).start()

        def block(j, carry):
            way, core = j % 2, j // 2
            chip = z + s * (2 * way - 1)
            here = jnp.logical_and(jnp.logical_and(chip >= 0, chip < nz), way * 1 <= s)
            slot = 2 * chip + core * (1 - c) + (1 - core) * c

            @pl.when(here)
            def _():
                @pl.when(core == 1)
                def _():
                    gather_wait(w, slot)

                columns = pl.ds(pl.multiple_of(slot * rows, rows), rows)
                acc[w] += jnp.dot(
                    x[w // 2, :, columns], w_all[w, slot], preferred_element_type=jnp.float32
                )

            return carry

        lax.fori_loop(0, 4, block, 0)

    def gather(w):
        def body(s, carry):
            gather_step(w, s)
            return carry

        lax.fori_loop(0, nz, body, 0)

    def by_rows(body):
        height = 32

        def step(i, carry):
            body(pl.ds(pl.multiple_of(i * height, height), height))
            return carry

        lax.fori_loop(0, x.shape[1] // height, step, 0)

    def term(g, slot):
        columns = pl.ds(pl.multiple_of(slot * rows, rows), rows)
        return token_product(x[g // 2, :, columns], cots[g])

    def sibling_copy(g, chip):
        return pltpu.make_async_remote_copy(
            src_ref=sib_out.at[g, chip], dst_ref=sib_in.at[g, chip],
            send_sem=sib_send.at[g, chip], recv_sem=sib_recv.at[g, chip],
            device_id={"fs": other}, device_id_type=MESH,
        )

    def line_copy(g, way, chip):
        return pltpu.make_async_remote_copy(
            src_ref=line_out.at[g, chip], dst_ref=line_in.at[g, way, chip],
            send_sem=line_send.at[g, chip], recv_sem=line_recv.at[g, way, chip],
            device_id={"fs": me + 2 - 4 * way}, device_id_type=MESH,
        )

    def pair_sum(g, chip):
        sib_out[g, chip] = term(g, 2 * chip + 1 - c).astype(jnp.bfloat16)
        sibling_copy(g, chip).start()
        own = term(g, 2 * chip + c)
        sibling_copy(g, chip).wait_recv()
        return own + sib_in[g, chip].astype(jnp.float32)

    def reduce_step(g, k):
        def one(j, carry):
            way = jnp.where(z * 2 >= nz, 1 - j, j)
            chip = jnp.where(way == RIGHT, nz - k, k - 1)
            active = jnp.where(way == RIGHT, chip - z, z - chip) > 0
            behind = jnp.where(way == RIGHT, z, nz - 1 - z) > 0

            @pl.when(active)
            def _():
                total[...] = pair_sum(g, chip)

                @pl.when(behind)
                def _():
                    line_copy(g, way, chip).wait_recv()
                    total[...] += line_in[g, way, chip].astype(jnp.float32)

                line_out[g, chip] = total[...].astype(jnp.bfloat16)
                line_copy(g, way, chip).start()

            return carry

        lax.fori_loop(0, 2, one, 0)

    def reduce_own(g):
        out[g] = pair_sum(g, z)

    def reduce_final(g):
        @pl.when(has_left)
        def _():
            line_copy(g, RIGHT, z).wait_recv()
            out[g] += line_in[g, RIGHT, z].astype(jnp.float32)

        @pl.when(has_right)
        def _():
            line_copy(g, LEFT, z).wait_recv()
            out[g] += line_in[g, LEFT, z].astype(jnp.float32)

    def reduce_down(now):
        @pl.when(now)
        def _():
            def body(k, carry):
                reduce_step(DOWN, k)
                return carry

            lax.fori_loop(1, nz, body, 0)

    def input_copy(peer, source):
        return pltpu.make_async_remote_copy(
            src_ref=ig_part.at[peer], dst_ref=ig_in.at[source],
            send_sem=ig_send.at[peer], recv_sem=ig_recv.at[source],
            device_id={"tp": peer}, device_id_type=MESH,
        )

    def input_part(step):
        peer = lax.rem(tp + 1 + step, n_tp)

        def piece(i, carry):
            slot = peer * pieces + i
            value = row_product(cots[GATE], w_all[GATE, slot])
            value = value + row_product(cots[UP], w_all[UP, slot])
            ig_part[peer, :, pl.ds(pl.multiple_of(i * rows, rows), rows)] = value.astype(jnp.bfloat16)
            return carry

        lax.fori_loop(0, pieces, piece, 0)

        @pl.when(step < n_tp - 1)
        def _():
            input_copy(peer, tp).start()

    def first_two(w, carry):
        gather(w)
        return carry

    lax.fori_loop(0, 2, first_two, 0)

    def make_hidden(r):
        gate = acc[GATE, r, :]
        sig = jax.nn.sigmoid(gate)
        act = gate * sig
        up = acc[UP, r, :]
        cots[DOWN, r, :] = (act * up).astype(jnp.bfloat16)
        acc[UP, r, :] = up * sig * (1.0 + gate * (1.0 - sig))
        acc[GATE, r, :] = act

    by_rows(make_hidden)
    reduce_down(is_end)
    gather(DOWN)
    reduce_down(jnp.logical_not(is_end))

    def make_cots(r):
        hidden_grad = acc[DOWN, r, :]
        cots[GATE, r, :] = (hidden_grad * acc[UP, r, :]).astype(jnp.bfloat16)
        cots[UP, r, :] = (hidden_grad * acc[GATE, r, :]).astype(jnp.bfloat16)

    by_rows(make_cots)

    def last_two(t, carry):
        @pl.when(t < 2 * (nz - 1))
        def _():
            reduce_step(t // max(nz - 1, 1), t % max(nz - 1, 1) + 1)

        @pl.when(t < n_tp)
        def _():
            input_part(t)

        return carry

    lax.fori_loop(0, max(2 * (nz - 1), n_tp), last_two, 0)

    def owns(g, carry):
        reduce_own(g)
        return carry

    lax.fori_loop(0, 3, owns, 0)

    ig_in[tp] = ig_part[tp]
    for step in range(1, n_tp):
        source = lax.rem(tp + step, n_tp)
        input_copy(source, source).wait_recv()
    for half in range(2):
        height = ig_out.shape[0] // 2
        r = pl.ds(half * height, height)
        value = ig_in[0, r, :].astype(jnp.float32)
        for source in range(1, n_tp):
            value = value + ig_in[source, r, :].astype(jnp.float32)
        ig_out[r, :] = value.astype(ig_out.dtype)

    def finals(i, carry):
        reduce_final(lax.rem(i + 2, 3))
        return carry

    lax.fori_loop(0, 3, finals, 0)

    def drain(i, carry):
        g, chip = i // nz, i % nz
        gather_copy(g, chip, SIBLING).wait_send()
        sibling_copy(g, chip).wait_send()

        @pl.when(jnp.logical_and(has_right, chip <= z))
        def _():
            gather_copy(g, chip, RIGHT).wait_send()

        @pl.when(jnp.logical_and(has_left, chip >= z))
        def _():
            gather_copy(g, chip, LEFT).wait_send()

        @pl.when(chip != z)
        def _():
            way = jnp.where(chip > z, RIGHT, LEFT)
            line_copy(g, way, chip).wait_send()

        return carry

    lax.fori_loop(0, 3 * nz, drain, 0)
    for step in range(1, n_tp):
        input_copy(lax.rem(tp + step, n_tp), tp).wait_send()


def fused_shards(tokens, cotangent, gate_weight, up_weight, down_weight):
    n, n_tp = lax.axis_size("fs"), lax.axis_size("tp")
    nz = n // 2
    count, width = tokens.shape
    rows, hidden = gate_weight.shape
    share = width // n_tp
    bf16, f32 = jnp.bfloat16, jnp.float32
    dma = pltpu.SemaphoreType.DMA
    input_grad, grads = pl.pallas_call(
        functools.partial(kernel, n, n_tp),
        out_shape=(
            jax.ShapeDtypeStruct((count, share), bf16),
            jax.ShapeDtypeStruct((3, rows, hidden), f32),
        ),
        in_specs=[pl.BlockSpec(memory_space=pl.ANY)] * 5,
        out_specs=(pl.BlockSpec(memory_space=pltpu.VMEM),) * 2,
        scratch_shapes=[
            pltpu.VMEM((2, count, width), bf16),
            pltpu.VMEM((3, n, rows, hidden), bf16),
            pltpu.VMEM((3, count, hidden), f32),
            pltpu.VMEM((3, count, hidden), bf16),
            pltpu.VMEM((3, nz, rows, hidden), bf16),
            pltpu.VMEM((3, nz, rows, hidden), bf16),
            pltpu.VMEM((3, nz, rows, hidden), bf16),
            pltpu.VMEM((3, 2, nz, rows, hidden), bf16),
            pltpu.VMEM((rows, hidden), f32),
            pltpu.VMEM((n_tp, count, share), bf16),
            pltpu.VMEM((n_tp, count, share), bf16),
            dma((5,)),
            dma((3, 3, nz)),
            dma((3, n)),
            dma((3, nz)),
            dma((3, nz)),
            dma((3, nz)),
            dma((3, 2, nz)),
            dma((n_tp,)),
            dma((n_tp,)),
        ],
        compiler_params=pltpu.CompilerParams(
            collective_id=0, has_side_effects=True, vmem_limit_bytes=67043328
        ),
    )(tokens, cotangent, gate_weight, up_weight, down_weight)
    return input_grad, grads[0], grads[1], grads[2]


def shards(tokens, cotangent, gate_weight, up_weight, down_weight):
    n, n_tp = lax.axis_size("fs"), lax.axis_size("tp")
    rows = gate_weight.shape[0]
    share = tokens.shape[1] // n_tp
    if n % 2 == 0 and rows % 128 == 0 and share % rows == 0 and n <= 8:
        return fused_shards(tokens, cotangent, gate_weight, up_weight, down_weight)
    return plain_shards(tokens, cotangent, gate_weight, up_weight, down_weight)


def solution(mesh):
    in_specs = (P("fs", None), P("fs", None), P("fs", "tp"), P("fs", "tp"), P("fs", "tp"))
    out_specs = (P("fs", "tp"), P("fs", "tp"), P("fs", "tp"), P("fs", "tp"))
    return jax.shard_map(shards, mesh=mesh, in_specs=in_specs, out_specs=out_specs, check_vma=False)
```

```python
import functools

import jax
import jax.numpy as jnp
from jax import lax
from jax.experimental import pallas as pl
from jax.experimental.pallas import tpu as pltpu
from jax.sharding import PartitionSpec as P


def row_product(left, right):
    return lax.dot_general(
        left, right, (((1,), (1,)), ((), ())), preferred_element_type=jnp.float32
    )


def token_product(left, right):
    return lax.dot_general(
        left, right, (((0,), (0,)), ((), ())), preferred_element_type=jnp.float32
    )


def owner_sum(received, groups):
    return received.reshape(groups, received.shape[0] // groups, received.shape[1]).sum(axis=0)


def plain_shards(tokens, cotangent, gate_weight, up_weight, down_weight):
    groups = lax.axis_size("fs")
    whole_gate, whole_up, whole_down = (
        lax.all_gather(gate_weight, "fs", axis=0, tiled=True),
        lax.all_gather(up_weight, "fs", axis=0, tiled=True),
        lax.all_gather(down_weight, "fs", axis=0, tiled=True),
    )
    gate = jnp.dot(tokens, whole_gate, preferred_element_type=jnp.float32)
    up = jnp.dot(tokens, whole_up, preferred_element_type=jnp.float32)
    hidden_grad = jnp.dot(cotangent, whole_down, preferred_element_type=jnp.float32)
    sig = jax.nn.sigmoid(gate)
    act = gate * sig
    hidden = (act * up).astype(jnp.bfloat16)
    gate_cot = (hidden_grad * up * sig * (1.0 + gate * (1.0 - sig))).astype(jnp.bfloat16)
    up_cot = (hidden_grad * act).astype(jnp.bfloat16)
    partial_value = row_product(gate_cot, whole_gate) + row_product(up_cot, whole_up)
    input_grad = lax.psum_scatter(
        partial_value.astype(jnp.bfloat16), "tp", scatter_dimension=1, tiled=True
    )
    gate_term = token_product(tokens, gate_cot)
    gate_grad = owner_sum(
        lax.all_to_all(
            gate_term.astype(jnp.bfloat16), "fs", split_axis=0, concat_axis=0, tiled=True
        ).astype(gate_term.dtype),
        groups,
    )
    up_term = token_product(tokens, up_cot)
    up_grad = owner_sum(
        lax.all_to_all(
            up_term.astype(jnp.bfloat16), "fs", split_axis=0, concat_axis=0, tiled=True
        ).astype(up_term.dtype),
        groups,
    )
    down_term = token_product(cotangent, hidden)
    down_grad = owner_sum(
        lax.all_to_all(
            down_term.astype(jnp.bfloat16), "fs", split_axis=0, concat_axis=0, tiled=True
        ).astype(down_term.dtype),
        groups,
    )
    return (input_grad, gate_grad, up_grad, down_grad)


MESH = pl.DeviceIdType.MESH
GATE, UP, DOWN = 0, 1, 2
RIGHT, LEFT, SIBLING = 0, 1, 2


def kernel(
    n, n_tp, parts, tok, cot, gw, uw, dw, ig_out, gate_out, up_out, down_out,
    x, w_all, acc, cots, own_sum, sib_out, sib_in, line_out, line_in, total, ig_part, ig_in,
    local_sem, ag_send, ag_recv, sib_send, sib_recv, line_send, line_recv, ig_send, ig_recv,
):
    me, tp = lax.axis_index("fs"), lax.axis_index("tp")
    z, c = me // 2, me % 2
    nz = n // 2
    other = 2 * z + 1 - c
    rows = gw.shape[1]
    height = gw.shape[0] // parts
    own_columns = ig_out.shape[1]
    pieces = own_columns // rows
    has_left, has_right = z > 0, z < nz - 1
    is_end = jnp.logical_or(z == 0, z == nz - 1)

    def weight_load(t):
        piece = pl.ds((t // 3) * height, height)
        return pltpu.make_async_copy(
            (gw, uw, dw)[t % 3].at[piece, :], w_all.at[t, me], local_sem.at[t]
        )

    loads = [weight_load(t) for t in range(3 * parts)]
    loads += [
        pltpu.make_async_copy(tok, x.at[0], local_sem.at[3 * parts]),
        pltpu.make_async_copy(cot, x.at[1], local_sem.at[3 * parts + 1]),
    ]
    for load in loads:
        load.start()

    barrier = pltpu.get_barrier_semaphore()
    pl.semaphore_signal(barrier, inc=1, device_id={"fs": other}, device_id_type=MESH)
    for step in range(1, n_tp):
        pl.semaphore_signal(
            barrier, inc=1, device_id={"tp": lax.rem(tp + step, n_tp)}, device_id_type=MESH
        )

    @pl.when(has_right)
    def _():
        pl.semaphore_signal(barrier, inc=1, device_id={"fs": me + 2}, device_id_type=MESH)

    @pl.when(has_left)
    def _():
        pl.semaphore_signal(barrier, inc=1, device_id={"fs": me - 2}, device_id_type=MESH)

    pl.semaphore_wait(barrier, n_tp + has_left.astype(jnp.int32) + has_right.astype(jnp.int32))

    def gather_copy(w, chip, way):
        slot = 2 * chip + c
        device = (me + 2, me - 2, other)[way]
        return pltpu.make_async_remote_copy(
            src_ref=w_all.at[w, slot], dst_ref=w_all.at[w, slot],
            send_sem=ag_send.at[w, way, chip], recv_sem=ag_recv.at[w, slot],
            device_id={"fs": device}, device_id_type=MESH,
        )

    def gather_wait(w, slot):
        pltpu.make_async_remote_copy(
            src_ref=w_all.at[w, slot], dst_ref=w_all.at[w, slot],
            send_sem=ag_send.at[w, SIBLING, 0], recv_sem=ag_recv.at[w, slot],
            device_id={"fs": other}, device_id_type=MESH,
        ).wait_recv()

    for t in range(3 * parts):
        loads[t].wait()

        @pl.when(jnp.logical_and(has_right, jnp.logical_or(z == 0, t == 0)))
        def _():
            gather_copy(t, z, RIGHT).start()

        @pl.when(jnp.logical_and(has_left, jnp.logical_or(z == nz - 1, t == 0)))
        def _():
            gather_copy(t, z, LEFT).start()

        gather_copy(t, z, SIBLING).start()
    loads[3 * parts].wait()
    loads[3 * parts + 1].wait()

    def gather_step(w, s):
        @pl.when(jnp.logical_and(s > 0, z - s >= 0))
        def _():
            gather_wait(w, me - 2 * s)

            @pl.when(has_right)
            def _():
                gather_copy(w, z - s, RIGHT).start()

            gather_copy(w, z - s, SIBLING).start()

        @pl.when(jnp.logical_and(s > 0, z + s < nz))
        def _():
            gather_wait(w, me + 2 * s)

            @pl.when(has_left)
            def _():
                gather_copy(w, z + s, LEFT).start()

            gather_copy(w, z + s, SIBLING).start()

        more = jnp.logical_and(w < 3 * parts - 1, jnp.logical_not(is_end))

        @pl.when(jnp.logical_and(more, s == z))
        def _():
            gather_copy(w + 1, z, RIGHT).start()

        @pl.when(jnp.logical_and(more, s == nz - 1 - z))
        def _():
            gather_copy(w + 1, z, LEFT).start()

        def block(j, carry):
            way, core = j % 2, j // 2
            chip = z + s * (2 * way - 1)
            here = jnp.logical_and(jnp.logical_and(chip >= 0, chip < nz), way * 1 <= s)
            slot = 2 * chip + core * (1 - c) + (1 - core) * c

            @pl.when(here)
            def _():
                @pl.when(core == 1)
                def _():
                    gather_wait(w, slot)

                columns = pl.ds(pl.multiple_of(slot * rows, rows), rows)
                kind = w % 3
                acc[kind] += row_product(w_all[w, slot], x[kind // 2, :, columns])

            return carry

        lax.fori_loop(0, 4, block, 0)

    def gather(w):
        def body(s, carry):
            gather_step(w, s)
            return carry

        lax.fori_loop(0, nz, body, 0)

    def by_rows(body):
        strip = 16

        def step(i, carry):
            body(pl.ds(pl.multiple_of(i * strip, strip), strip))
            return carry

        lax.fori_loop(0, height // strip, step, 0)

    def term(g, slot):
        columns = pl.ds(pl.multiple_of(slot * rows, rows), rows)
        return jnp.dot(
            cots[g], x[(g % 3) // 2, :, columns], preferred_element_type=jnp.float32
        )

    def sibling_copy(g, chip):
        return pltpu.make_async_remote_copy(
            src_ref=sib_out.at[g, chip], dst_ref=sib_in.at[g, chip],
            send_sem=sib_send.at[g, chip], recv_sem=sib_recv.at[g, chip],
            device_id={"fs": other}, device_id_type=MESH,
        )

    def line_copy(g, way, chip):
        return pltpu.make_async_remote_copy(
            src_ref=line_out.at[g, chip], dst_ref=line_in.at[g, way, chip],
            send_sem=line_send.at[g, chip], recv_sem=line_recv.at[g, way, chip],
            device_id={"fs": me + 2 - 4 * way}, device_id_type=MESH,
        )

    def sibling_term(g, chip):
        sib_out[g, chip] = term(g, 2 * chip + 1 - c).astype(jnp.bfloat16)
        sibling_copy(g, chip).start()

    def pair_sum(g, chip):
        own = term(g, 2 * chip + c)
        sibling_copy(g, chip).wait_recv()
        return own + sib_in[g, chip].astype(jnp.float32)

    def each_way(k, body):
        def one(j, carry):
            way = jnp.where(z * 2 >= nz, 1 - j, j)
            chip = jnp.where(way == RIGHT, nz - k, k - 1)
            active = jnp.where(way == RIGHT, chip - z, z - chip) > 0

            @pl.when(active)
            def _():
                body(way, chip)

            return carry

        lax.fori_loop(0, 2, one, 0)

    def sibling_terms(g):
        def body(k, carry):
            each_way(k, lambda way, chip: sibling_term(g, chip))
            return carry

        lax.fori_loop(1, nz, body, 0)
        sibling_term(g, z)

    def reduce_step(g, k):
        def one(way, chip):
            behind = jnp.where(way == RIGHT, z, nz - 1 - z) > 0
            total[...] = pair_sum(g, chip)

            @pl.when(behind)
            def _():
                line_copy(g, way, chip).wait_recv()
                total[...] += line_in[g, way, chip].astype(jnp.float32)

            line_out[g, chip] = total[...].astype(jnp.bfloat16)
            line_copy(g, way, chip).start()

        each_way(k, one)

    def reduce_own(g):
        own_sum[g] = pair_sum(g, z)

    def reduce_final(g):
        @pl.when(has_left)
        def _():
            line_copy(g, RIGHT, z).wait_recv()
            own_sum[g] += line_in[g, RIGHT, z].astype(jnp.float32)

        @pl.when(has_right)
        def _():
            line_copy(g, LEFT, z).wait_recv()
            own_sum[g] += line_in[g, LEFT, z].astype(jnp.float32)

        piece = pl.ds((g // 3) * height, height)
        (gate_out, up_out, down_out)[g % 3][piece, :] = own_sum[g]

    def reduce_all(g, now):
        @pl.when(now)
        def _():
            sibling_terms(g)

            def body(k, carry):
                reduce_step(g, k)
                return carry

            lax.fori_loop(1, nz, body, 0)
            reduce_own(g)

    def input_copy(peer, source):
        return pltpu.make_async_remote_copy(
            src_ref=ig_part.at[peer], dst_ref=ig_in.at[source],
            send_sem=ig_send.at[peer], recv_sem=ig_recv.at[source],
            device_id={"tp": peer}, device_id_type=MESH,
        )

    def input_part(step):
        peer = lax.rem(tp + 1 + step, n_tp)

        def piece(i, carry):
            slot = peer * pieces + i
            value = token_product(cots[GATE], w_all[GATE, slot])
            for t in [t for t in range(1, 3 * parts) if t % 3 != DOWN]:
                value = value + token_product(cots[t], w_all[t, slot])
            ig_part[peer, :, pl.ds(pl.multiple_of(i * rows, rows), rows)] = value.astype(jnp.bfloat16)
            return carry

        lax.fori_loop(0, pieces, piece, 0)

        @pl.when(step < n_tp - 1)
        def _():
            input_copy(peer, tp).start()

    def make_hidden(t):
        def strip(r):
            gate = acc[GATE, r, :]
            sig = jax.nn.sigmoid(gate)
            act = gate * sig
            up = acc[UP, r, :]
            cots[t + 1, r, :] = (act * up).astype(jnp.bfloat16)
            acc[UP, r, :] = up * sig * (1.0 + gate * (1.0 - sig))
            acc[GATE, r, :] = act

        by_rows(strip)

    def make_cots(t):
        def strip(r):
            hidden_grad = acc[DOWN, r, :]
            cots[t - 2, r, :] = (hidden_grad * acc[UP, r, :]).astype(jnp.bfloat16)
            cots[t - 1, r, :] = (hidden_grad * acc[GATE, r, :]).astype(jnp.bfloat16)

        by_rows(strip)

    def gather_and_reduce(t, carry):
        kind = t % 3
        g = jnp.where(kind == DOWN, t, t - 3)
        acc[kind] = jnp.zeros(acc.shape[1:], acc.dtype)
        reduce_all(g, jnp.logical_and(g >= 0, is_end))
        gather(t)
        reduce_all(g, jnp.logical_and(g >= 0, jnp.logical_not(is_end)))

        @pl.when(kind == UP)
        def _():
            make_hidden(t)

        @pl.when(kind == DOWN)
        def _():
            make_cots(t)

        return carry

    lax.fori_loop(0, 3 * parts, gather_and_reduce, 0)
    last = 3 * parts - 3
    steps = max(nz - 1, 1)

    def last_two(i, carry):
        g = last + i // steps

        @pl.when(jnp.logical_and(i < 2 * steps, i % steps == 0))
        def _():
            sibling_terms(g)

        @pl.when(i < 2 * (nz - 1))
        def _():
            reduce_step(g, i % steps + 1)

        @pl.when(i < n_tp)
        def _():
            input_part(i)

        return carry

    lax.fori_loop(0, max(2 * steps, n_tp), last_two, 0)
    reduce_own(last)
    reduce_own(last + 1)

    ig_in[tp] = ig_part[tp]
    for step in range(1, n_tp):
        source = lax.rem(tp + step, n_tp)
        input_copy(source, source).wait_recv()
    for half in range(2):
        strip = ig_out.shape[0] // 2
        r = pl.ds(half * strip, strip)
        value = ig_in[0, r, :].astype(jnp.float32)
        for source in range(1, n_tp):
            value = value + ig_in[source, r, :].astype(jnp.float32)
        ig_out[r, :] = value.astype(ig_out.dtype)

    for p in range(parts):
        for kind in (DOWN, GATE, UP):
            reduce_final(3 * p + kind)

    def drain(i, carry):
        g, chip = i // nz, i % nz
        gather_copy(g, chip, SIBLING).wait_send()
        sibling_copy(g, chip).wait_send()

        @pl.when(jnp.logical_and(has_right, chip <= z))
        def _():
            gather_copy(g, chip, RIGHT).wait_send()

        @pl.when(jnp.logical_and(has_left, chip >= z))
        def _():
            gather_copy(g, chip, LEFT).wait_send()

        @pl.when(chip != z)
        def _():
            way = jnp.where(chip > z, RIGHT, LEFT)
            line_copy(g, way, chip).wait_send()

        return carry

    lax.fori_loop(0, 3 * parts * nz, drain, 0)
    for step in range(1, n_tp):
        input_copy(lax.rem(tp + step, n_tp), tp).wait_send()


PARTS = 1


def fused_shards(tokens, cotangent, gate_weight, up_weight, down_weight):
    n, n_tp = lax.axis_size("fs"), lax.axis_size("tp")
    nz = n // 2
    count, width = tokens.shape
    rows, hidden = gate_weight.shape
    height = hidden // PARTS
    pieces = 3 * PARTS
    share = width // n_tp
    bf16, f32 = jnp.bfloat16, jnp.float32
    dma = pltpu.SemaphoreType.DMA
    input_grad, gate_grad, up_grad, down_grad = pl.pallas_call(
        functools.partial(kernel, n, n_tp, PARTS),
        out_shape=(
            jax.ShapeDtypeStruct((count, share), bf16),
        ) + (jax.ShapeDtypeStruct((hidden, rows), f32),) * 3,
        in_specs=[pl.BlockSpec(memory_space=pl.ANY)] * 5,
        out_specs=(pl.BlockSpec(memory_space=pltpu.VMEM),) * 4,
        scratch_shapes=[
            pltpu.VMEM((2, count, width), bf16),
            pltpu.VMEM((pieces, n, height, rows), bf16),
            pltpu.VMEM((3, height, count), f32),
            pltpu.VMEM((pieces, height, count), bf16),
            pltpu.VMEM((pieces, height, rows), f32),
            pltpu.VMEM((pieces, nz, height, rows), bf16),
            pltpu.VMEM((pieces, nz, height, rows), bf16),
            pltpu.VMEM((pieces, nz, height, rows), bf16),
            pltpu.VMEM((pieces, 2, nz, height, rows), bf16),
            pltpu.VMEM((height, rows), f32),
            pltpu.VMEM((n_tp, count, share), bf16),
            pltpu.VMEM((n_tp, count, share), bf16),
            dma((pieces + 2,)),
            dma((pieces, 3, nz)),
            dma((pieces, n)),
            dma((pieces, nz)),
            dma((pieces, nz)),
            dma((pieces, nz)),
            dma((pieces, 2, nz)),
            dma((n_tp,)),
            dma((n_tp,)),
        ],
        compiler_params=pltpu.CompilerParams(
            collective_id=0, has_side_effects=True, vmem_limit_bytes=67043328
        ),
    )(tokens, cotangent, gate_weight.T, up_weight.T, down_weight.T)
    return input_grad, gate_grad.T, up_grad.T, down_grad.T


def shards(tokens, cotangent, gate_weight, up_weight, down_weight):
    n, n_tp = lax.axis_size("fs"), lax.axis_size("tp")
    rows = gate_weight.shape[0]
    share = tokens.shape[1] // n_tp
    if n % 2 == 0 and rows % 128 == 0 and share % rows == 0 and n <= 8 and (
        gate_weight.shape[1] % (16 * PARTS) == 0
    ):
        return fused_shards(tokens, cotangent, gate_weight, up_weight, down_weight)
    return plain_shards(tokens, cotangent, gate_weight, up_weight, down_weight)


def solution(mesh):
    in_specs = (P("fs", None), P("fs", None), P("fs", "tp"), P("fs", "tp"), P("fs", "tp"))
    out_specs = (P("fs", "tp"), P("fs", "tp"), P("fs", "tp"), P("fs", "tp"))
    return jax.shard_map(shards, mesh=mesh, in_specs=in_specs, out_specs=out_specs, check_vma=False)
```

```python
import functools

import jax
import jax.numpy as jnp
from jax import lax
from jax.experimental import pallas as pl
from jax.experimental.pallas import tpu as pltpu
from jax.sharding import PartitionSpec as P


def row_product(left, right):
    return lax.dot_general(
        left, right, (((1,), (1,)), ((), ())), preferred_element_type=jnp.float32
    )


def token_product(left, right):
    return lax.dot_general(
        left, right, (((0,), (0,)), ((), ())), preferred_element_type=jnp.float32
    )


def owner_sum(received, groups):
    return received.reshape(groups, received.shape[0] // groups, received.shape[1]).sum(axis=0)


def plain_shards(tokens, cotangent, gate_weight, up_weight, down_weight):
    groups = lax.axis_size("fs")
    whole_gate, whole_up, whole_down = (
        lax.all_gather(gate_weight, "fs", axis=0, tiled=True),
        lax.all_gather(up_weight, "fs", axis=0, tiled=True),
        lax.all_gather(down_weight, "fs", axis=0, tiled=True),
    )
    gate = jnp.dot(tokens, whole_gate, preferred_element_type=jnp.float32)
    up = jnp.dot(tokens, whole_up, preferred_element_type=jnp.float32)
    hidden_grad = jnp.dot(cotangent, whole_down, preferred_element_type=jnp.float32)
    sig = jax.nn.sigmoid(gate)
    act = gate * sig
    hidden = (act * up).astype(jnp.bfloat16)
    gate_cot = (hidden_grad * up * sig * (1.0 + gate * (1.0 - sig))).astype(jnp.bfloat16)
    up_cot = (hidden_grad * act).astype(jnp.bfloat16)
    partial_value = row_product(gate_cot, whole_gate) + row_product(up_cot, whole_up)
    input_grad = lax.psum_scatter(
        partial_value.astype(jnp.bfloat16), "tp", scatter_dimension=1, tiled=True
    )
    gate_term = token_product(tokens, gate_cot)
    gate_grad = owner_sum(
        lax.all_to_all(
            gate_term.astype(jnp.bfloat16), "fs", split_axis=0, concat_axis=0, tiled=True
        ).astype(gate_term.dtype),
        groups,
    )
    up_term = token_product(tokens, up_cot)
    up_grad = owner_sum(
        lax.all_to_all(
            up_term.astype(jnp.bfloat16), "fs", split_axis=0, concat_axis=0, tiled=True
        ).astype(up_term.dtype),
        groups,
    )
    down_term = token_product(cotangent, hidden)
    down_grad = owner_sum(
        lax.all_to_all(
            down_term.astype(jnp.bfloat16), "fs", split_axis=0, concat_axis=0, tiled=True
        ).astype(down_term.dtype),
        groups,
    )
    return (input_grad, gate_grad, up_grad, down_grad)


MESH = pl.DeviceIdType.MESH
LAG = 2
GATE, UP, DOWN = 0, 1, 2
RIGHT, LEFT, SIBLING = 0, 1, 2


def kernel(
    n, n_tp, parts, tok, cot, gw, uw, dw, ig_out, gate_out, up_out, down_out,
    x, w_all, acc, cots, own_sum, sib_out, sib_in, line_out, line_in, total, ig_part, ig_in,
    local_sem, ag_send, ag_recv, sib_send, sib_recv, line_send, line_recv, ig_send, ig_recv,
):
    me, tp = lax.axis_index("fs"), lax.axis_index("tp")
    z, c = me // 2, me % 2
    nz = n // 2
    other = 2 * z + 1 - c
    rows = gw.shape[1]
    height = gw.shape[0] // parts
    own_columns = ig_out.shape[1]
    pieces = own_columns // rows
    has_left, has_right = z > 0, z < nz - 1
    is_end = jnp.logical_or(z == 0, z == nz - 1)

    def weight_load(t):
        piece = pl.ds((t // 3) * height, height)
        return pltpu.make_async_copy(
            (gw, uw, dw)[t % 3].at[piece, :], w_all.at[t, me], local_sem.at[t]
        )

    loads = [weight_load(t) for t in range(3 * parts)]
    loads += [
        pltpu.make_async_copy(tok, x.at[0], local_sem.at[3 * parts]),
        pltpu.make_async_copy(cot, x.at[1], local_sem.at[3 * parts + 1]),
    ]
    for load in loads:
        load.start()

    barrier = pltpu.get_barrier_semaphore()
    pl.semaphore_signal(barrier, inc=1, device_id={"fs": other}, device_id_type=MESH)
    for step in range(1, n_tp):
        pl.semaphore_signal(
            barrier, inc=1, device_id={"tp": lax.rem(tp + step, n_tp)}, device_id_type=MESH
        )

    @pl.when(has_right)
    def _():
        pl.semaphore_signal(barrier, inc=1, device_id={"fs": me + 2}, device_id_type=MESH)

    @pl.when(has_left)
    def _():
        pl.semaphore_signal(barrier, inc=1, device_id={"fs": me - 2}, device_id_type=MESH)

    pl.semaphore_wait(barrier, n_tp + has_left.astype(jnp.int32) + has_right.astype(jnp.int32))

    def gather_copy(w, chip, way):
        slot = 2 * chip + c
        device = (me + 2, me - 2, other)[way]
        return pltpu.make_async_remote_copy(
            src_ref=w_all.at[w, slot], dst_ref=w_all.at[w, slot],
            send_sem=ag_send.at[w, way, chip], recv_sem=ag_recv.at[w, slot],
            device_id={"fs": device}, device_id_type=MESH,
        )

    def gather_wait(w, slot):
        pltpu.make_async_remote_copy(
            src_ref=w_all.at[w, slot], dst_ref=w_all.at[w, slot],
            send_sem=ag_send.at[w, SIBLING, 0], recv_sem=ag_recv.at[w, slot],
            device_id={"fs": other}, device_id_type=MESH,
        ).wait_recv()

    for t in range(3 * parts):
        loads[t].wait()

        @pl.when(jnp.logical_and(has_right, jnp.logical_or(z == 0, t == 0)))
        def _():
            gather_copy(t, z, RIGHT).start()

        @pl.when(jnp.logical_and(has_left, jnp.logical_or(z == nz - 1, t == 0)))
        def _():
            gather_copy(t, z, LEFT).start()

        gather_copy(t, z, SIBLING).start()
    loads[3 * parts].wait()
    loads[3 * parts + 1].wait()

    def gather_step(w, s):
        @pl.when(jnp.logical_and(s > 0, z - s >= 0))
        def _():
            gather_wait(w, me - 2 * s)

            @pl.when(has_right)
            def _():
                gather_copy(w, z - s, RIGHT).start()

            gather_copy(w, z - s, SIBLING).start()

        @pl.when(jnp.logical_and(s > 0, z + s < nz))
        def _():
            gather_wait(w, me + 2 * s)

            @pl.when(has_left)
            def _():
                gather_copy(w, z + s, LEFT).start()

            gather_copy(w, z + s, SIBLING).start()

        more = jnp.logical_and(w < 3 * parts - 1, jnp.logical_not(is_end))

        @pl.when(jnp.logical_and(more, s == z))
        def _():
            gather_copy(w + 1, z, RIGHT).start()

        @pl.when(jnp.logical_and(more, s == nz - 1 - z))
        def _():
            gather_copy(w + 1, z, LEFT).start()

        def block(j, carry):
            way, core = j % 2, j // 2
            chip = z + s * (2 * way - 1)
            here = jnp.logical_and(jnp.logical_and(chip >= 0, chip < nz), way * 1 <= s)
            slot = 2 * chip + core * (1 - c) + (1 - core) * c

            @pl.when(here)
            def _():
                @pl.when(core == 1)
                def _():
                    gather_wait(w, slot)

                columns = pl.ds(pl.multiple_of(slot * rows, rows), rows)
                kind = w % 3
                acc[kind] += row_product(w_all[w, slot], x[kind // 2, :, columns])

            return carry

        lax.fori_loop(0, 4, block, 0)

    def gather(w):
        def body(s, carry):
            gather_step(w, s)
            return carry

        lax.fori_loop(0, nz, body, 0)

    def by_rows(body):
        strip = 16

        def step(i, carry):
            body(pl.ds(pl.multiple_of(i * strip, strip), strip))
            return carry

        lax.fori_loop(0, height // strip, step, 0)

    def term(g, slot):
        columns = pl.ds(pl.multiple_of(slot * rows, rows), rows)
        return jnp.dot(
            cots[g], x[(g % 3) // 2, :, columns], preferred_element_type=jnp.float32
        )

    def sibling_copy(g, chip):
        return pltpu.make_async_remote_copy(
            src_ref=sib_out.at[g, chip], dst_ref=sib_in.at[g, chip],
            send_sem=sib_send.at[g, chip], recv_sem=sib_recv.at[g, chip],
            device_id={"fs": other}, device_id_type=MESH,
        )

    def line_copy(g, way, chip):
        return pltpu.make_async_remote_copy(
            src_ref=line_out.at[g, chip], dst_ref=line_in.at[g, way, chip],
            send_sem=line_send.at[g, chip], recv_sem=line_recv.at[g, way, chip],
            device_id={"fs": me + 2 - 4 * way}, device_id_type=MESH,
        )

    def sibling_term(g, chip):
        sib_out[g, chip] = term(g, 2 * chip + 1 - c).astype(jnp.bfloat16)
        sibling_copy(g, chip).start()

    def pair_sum(g, chip):
        own = term(g, 2 * chip + c)
        sibling_copy(g, chip).wait_recv()
        return own + sib_in[g, chip].astype(jnp.float32)

    def each_way(k, body):
        def one(j, carry):
            way = jnp.where(z * 2 >= nz, 1 - j, j)
            chip = jnp.where(way == RIGHT, nz - k, k - 1)
            active = jnp.where(way == RIGHT, chip - z, z - chip) > 0

            @pl.when(active)
            def _():
                body(way, chip)

            return carry

        lax.fori_loop(0, 2, one, 0)

    def sibling_terms(g):
        def body(k, carry):
            each_way(k, lambda way, chip: sibling_term(g, chip))
            return carry

        lax.fori_loop(1, nz, body, 0)
        sibling_term(g, z)

    def reduce_step(g, k):
        def one(way, chip):
            behind = jnp.where(way == RIGHT, z, nz - 1 - z) > 0
            total[...] = pair_sum(g, chip)

            @pl.when(behind)
            def _():
                line_copy(g, way, chip).wait_recv()
                total[...] += line_in[g, way, chip].astype(jnp.float32)

            line_out[g, chip] = total[...].astype(jnp.bfloat16)
            line_copy(g, way, chip).start()

        each_way(k, one)

    def reduce_own(g):
        own_sum[g] = pair_sum(g, z)

    def reduce_final(g):
        @pl.when(has_left)
        def _():
            line_copy(g, RIGHT, z).wait_recv()
            own_sum[g] += line_in[g, RIGHT, z].astype(jnp.float32)

        @pl.when(has_right)
        def _():
            line_copy(g, LEFT, z).wait_recv()
            own_sum[g] += line_in[g, LEFT, z].astype(jnp.float32)

        piece = pl.ds((g // 3) * height, height)
        (gate_out, up_out, down_out)[g % 3][piece, :] = own_sum[g]

    def reduce_all(g, now):
        @pl.when(now)
        def _():
            sibling_terms(g)

            def body(k, carry):
                reduce_step(g, k)
                return carry

            lax.fori_loop(1, nz, body, 0)
            reduce_own(g)

    def input_copy(peer, source):
        return pltpu.make_async_remote_copy(
            src_ref=ig_part.at[peer], dst_ref=ig_in.at[source],
            send_sem=ig_send.at[peer], recv_sem=ig_recv.at[source],
            device_id={"tp": peer}, device_id_type=MESH,
        )

    def input_part(step):
        peer = lax.rem(tp + 1 + step, n_tp)

        def piece(i, carry):
            slot = peer * pieces + i
            value = token_product(cots[GATE], w_all[GATE, slot])
            for t in [t for t in range(1, 3 * parts) if t % 3 != DOWN]:
                value = value + token_product(cots[t], w_all[t, slot])
            ig_part[peer, :, pl.ds(pl.multiple_of(i * rows, rows), rows)] = value.astype(jnp.bfloat16)
            return carry

        lax.fori_loop(0, pieces, piece, 0)

        @pl.when(step < n_tp - 1)
        def _():
            input_copy(peer, tp).start()

    def make_hidden(t):
        def strip(r):
            gate = acc[GATE, r, :]
            sig = jax.nn.sigmoid(gate)
            act = gate * sig
            up = acc[UP, r, :]
            cots[t + 1, r, :] = (act * up).astype(jnp.bfloat16)
            acc[UP, r, :] = up * sig * (1.0 + gate * (1.0 - sig))
            acc[GATE, r, :] = act

        by_rows(strip)

    def make_cots(t):
        def strip(r):
            hidden_grad = acc[DOWN, r, :]
            cots[t - 2, r, :] = (hidden_grad * acc[UP, r, :]).astype(jnp.bfloat16)
            cots[t - 1, r, :] = (hidden_grad * acc[GATE, r, :]).astype(jnp.bfloat16)

        by_rows(strip)

    def in_turn(i):
        return 3 * (i // 3) + (i + 2) % 3

    def gather_and_reduce(t, carry):
        kind = t % 3
        g = jnp.where(kind == DOWN, t, t - 3)
        acc[kind] = jnp.zeros(acc.shape[1:], acc.dtype)
        reduce_all(g, jnp.logical_and(g >= 0, is_end))
        gather(t)
        turn = t - 2 - LAG
        reduce_all(in_turn(turn), jnp.logical_and(turn >= 0, jnp.logical_not(is_end)))

        @pl.when(kind == UP)
        def _():
            make_hidden(t)

        @pl.when(kind == DOWN)
        def _():
            make_cots(t)

        return carry

    lax.fori_loop(0, 3 * parts, gather_and_reduce, 0)
    last = 3 * parts - 3

    def catch_up(turn, carry):
        reduce_all(in_turn(turn), jnp.logical_not(is_end))
        return carry

    lax.fori_loop(max(3 * parts - 2 - LAG, 0), 3 * parts - 2, catch_up, 0)
    steps = max(nz - 1, 1)

    def last_two(i, carry):
        g = last + i // steps

        @pl.when(jnp.logical_and(i < 2 * steps, i % steps == 0))
        def _():
            sibling_terms(g)

        @pl.when(jnp.logical_and(i < n_tp, jnp.logical_not(is_end)))
        def _():
            input_part(i)

        @pl.when(i < 2 * (nz - 1))
        def _():
            reduce_step(g, i % steps + 1)

        @pl.when(jnp.logical_and(i < n_tp, is_end))
        def _():
            input_part(i)

        return carry

    lax.fori_loop(0, max(2 * steps, n_tp), last_two, 0)
    reduce_own(last)
    reduce_own(last + 1)

    ig_in[tp] = ig_part[tp]
    for step in range(1, n_tp):
        source = lax.rem(tp + step, n_tp)
        input_copy(source, source).wait_recv()
    for half in range(2):
        strip = ig_out.shape[0] // 2
        r = pl.ds(half * strip, strip)
        value = ig_in[0, r, :].astype(jnp.float32)
        for source in range(1, n_tp):
            value = value + ig_in[source, r, :].astype(jnp.float32)
        ig_out[r, :] = value.astype(ig_out.dtype)

    for p in range(parts):
        for kind in (DOWN, GATE, UP):
            reduce_final(3 * p + kind)

    def drain(i, carry):
        g, chip = i // nz, i % nz
        gather_copy(g, chip, SIBLING).wait_send()
        sibling_copy(g, chip).wait_send()

        @pl.when(jnp.logical_and(has_right, chip <= z))
        def _():
            gather_copy(g, chip, RIGHT).wait_send()

        @pl.when(jnp.logical_and(has_left, chip >= z))
        def _():
            gather_copy(g, chip, LEFT).wait_send()

        @pl.when(chip != z)
        def _():
            way = jnp.where(chip > z, RIGHT, LEFT)
            line_copy(g, way, chip).wait_send()

        return carry

    lax.fori_loop(0, 3 * parts * nz, drain, 0)
    for step in range(1, n_tp):
        input_copy(lax.rem(tp + step, n_tp), tp).wait_send()


PARTS = 2


def fused_shards(tokens, cotangent, gate_weight, up_weight, down_weight):
    n, n_tp = lax.axis_size("fs"), lax.axis_size("tp")
    nz = n // 2
    count, width = tokens.shape
    rows, hidden = gate_weight.shape
    height = hidden // PARTS
    pieces = 3 * PARTS
    share = width // n_tp
    bf16, f32 = jnp.bfloat16, jnp.float32
    dma = pltpu.SemaphoreType.DMA
    input_grad, gate_grad, up_grad, down_grad = pl.pallas_call(
        functools.partial(kernel, n, n_tp, PARTS),
        out_shape=(
            jax.ShapeDtypeStruct((count, share), bf16),
        ) + (jax.ShapeDtypeStruct((hidden, rows), f32),) * 3,
        in_specs=[pl.BlockSpec(memory_space=pl.ANY)] * 5,
        out_specs=(pl.BlockSpec(memory_space=pltpu.VMEM),) * 4,
        scratch_shapes=[
            pltpu.VMEM((2, count, width), bf16),
            pltpu.VMEM((pieces, n, height, rows), bf16),
            pltpu.VMEM((3, height, count), f32),
            pltpu.VMEM((pieces, height, count), bf16),
            pltpu.VMEM((pieces, height, rows), f32),
            pltpu.VMEM((pieces, nz, height, rows), bf16),
            pltpu.VMEM((pieces, nz, height, rows), bf16),
            pltpu.VMEM((pieces, nz, height, rows), bf16),
            pltpu.VMEM((pieces, 2, nz, height, rows), bf16),
            pltpu.VMEM((height, rows), f32),
            pltpu.VMEM((n_tp, count, share), bf16),
            pltpu.VMEM((n_tp, count, share), bf16),
            dma((pieces + 2,)),
            dma((pieces, 3, nz)),
            dma((pieces, n)),
            dma((pieces, nz)),
            dma((pieces, nz)),
            dma((pieces, nz)),
            dma((pieces, 2, nz)),
            dma((n_tp,)),
            dma((n_tp,)),
        ],
        compiler_params=pltpu.CompilerParams(
            collective_id=0, has_side_effects=True, vmem_limit_bytes=67043328
        ),
    )(tokens, cotangent, gate_weight.T, up_weight.T, down_weight.T)
    return input_grad, gate_grad.T, up_grad.T, down_grad.T


def shards(tokens, cotangent, gate_weight, up_weight, down_weight):
    n, n_tp = lax.axis_size("fs"), lax.axis_size("tp")
    rows = gate_weight.shape[0]
    share = tokens.shape[1] // n_tp
    if n % 2 == 0 and rows % 128 == 0 and share % rows == 0 and n <= 8 and (
        gate_weight.shape[1] % (16 * PARTS) == 0
    ):
        return fused_shards(tokens, cotangent, gate_weight, up_weight, down_weight)
    return plain_shards(tokens, cotangent, gate_weight, up_weight, down_weight)


def solution(mesh):
    in_specs = (P("fs", None), P("fs", None), P("fs", "tp"), P("fs", "tp"), P("fs", "tp"))
    out_specs = (P("fs", "tp"), P("fs", "tp"), P("fs", "tp"), P("fs", "tp"))
    return jax.shard_map(shards, mesh=mesh, in_specs=in_specs, out_specs=out_specs, check_vma=False)
```
